32 devices in a mesh: grp: 2 (over x), ep: 16 (over z, y, core).
Axes of the slice: x: 2, y: 2, z: 4, core: 2. Of those that a mesh axis runs over, the one named last changes fastest.
Arguments:
- tokens: bfloat16 [4096, 2048], P(('grp', 'ep')), parts along dimension 0, may hold values from -6 to 6
- routing: int32 [4096, 2], P(('grp', 'ep')), parts along dimension 0, may hold values from 0 to 3, all different within a row; in each aligned block of 128 rows (0 to 127, 128 to 255, ...) at most 80 rows name the same one
- gates: float32 [4096, 2], P(('grp', 'ep')), parts along dimension 0, may hold values from 0.2 to 1
- norm_gain: bfloat16 [2048], replicated, may hold values from 0.099609375 to 1.8984375
- w_gate: bfloat16 [16, 2048, 896], P('ep'), may hold values from -0.125 to 0.125
- w_up: bfloat16 [16, 2048, 896], P('ep'), may hold values from -0.125 to 0.125
- w_down: bfloat16 [16, 896, 2048], P('ep'), may hold values from -0.09375 to 0.09375
Outputs:
- mixed: bfloat16 [4096, 2048], P(('grp', 'ep')), parts along dimension 0
The draws below stay inside these ranges and needn't reach their ends.
There are 2 independent parts, one for each index of `grp`. The reference program is written for one: setup_inputs(seed, part) draws one part's arguments, and reference() takes and returns one part's arrays. A program takes and returns all parts, laid end to end along the dimension named above; an argument that names none is the same for every part. Nothing has to cross between parts.
Inputs may be any that keep to these rules, and one draw needn't show every extreme that they name: `routing`: each row names 2 different experts. Among the rows of one device at most 80 name any one expert, and in every draw some expert is named by exactly 80 rows of some device.
All inputs are finite; a program needn't handle non-finite values.
Results may differ from the reference program's by a relative error of at most 0.0078.
Values may be sent and summed in bfloat16 or wider, within the bound.
A program may use at most 128 MiB of HBM per device.

```python
import math
import jax
import jax.numpy as jnp
import numpy as np
from jax import lax

D = 2048
FF = 3584
TOP = 2
GROUP = 4
TOK_DEV = 128
EXPERTS = 4
CAP = 80
TOKENS = 2048
N_EP = 16


def levels(key, dims, pieces, low, top_value):
    factor_of, own = 1.0, jax.random.fold_in(key, 6)
    for axis_at, blocks in pieces:
        steps = jnp.exp(jax.random.uniform(jax.random.fold_in(own, axis_at), (blocks,), jnp.float32, low / len(pieces), top_value / len(pieces)))
        factor_of = factor_of * jnp.repeat(steps, dims[axis_at] // blocks).reshape([-1 if axis == axis_at else 1 for axis in range(len(dims))])
    return factor_of


def assign_block(own_key, own, number, rows, number_of, top, bound, lean):
    order = jax.random.permutation(own_key, number_of)
    heavy_load, common = load_shares(number_of, rows * top, bound, lean, True), load_shares(number_of, rows * top, bound, lean, False)
    places = jnp.arange(number_of)

    def named(sizes, offset_by):
        used = int((sizes > 0).sum())
        fixed = max(1, used // 4)
        passed = fixed + (places - fixed + offset_by * (used - fixed)) % max(1, number_of - fixed)
        return jnp.zeros((number_of,), jnp.int32).at[order[jnp.where(places < fixed, places, passed)]].set(jnp.asarray(sizes, jnp.int32))

    sizes = jnp.where(number % 4 == 0, named(heavy_load, number // 4), named(common, number - number // 4 - 1))
    mixed = jax.random.permutation(jax.random.fold_in(own, 3), number_of)
    donor, taker = mixed[0:number_of // 2 * 2:2], mixed[1:number_of // 2 * 2:2]
    room = jnp.minimum(sizes[donor] - 1, bound - sizes[taker]) // 2
    room = jnp.where((donor == order[0]) | (taker == order[0]) | (sizes[taker] == 0), 0, jnp.maximum(room, 0))
    passed = jax.random.randint(jax.random.fold_in(own, 4), (number_of // 2,), 0, 1 << 20) % (room + 1)
    sizes = sizes.at[donor].add(-passed).at[taker].add(passed)
    labels = jnp.searchsorted(jnp.cumsum(sizes), jnp.arange(rows * top), side="right").astype(jnp.int32)
    table = labels.reshape(top, rows).T
    table = table[jax.random.permutation(jax.random.fold_in(own, 1), rows)]
    offset_by = jax.random.randint(jax.random.fold_in(own, 2), (rows, 1), 0, top)
    return jnp.take_along_axis(table, (jnp.arange(top)[None, :] + offset_by) % top, axis=1)


def load_shares(number_of, total, bound, skew, full):
    portions = [(1 << 20) // math.isqrt(grade ** skew) + 1 for grade in range(1, number_of + 1)]
    largest = bound if full else min(bound, max(-(-total // number_of), total * portions[0] // sum(portions)))
    least = 1 if total - largest >= number_of - 1 else 0
    given, spare = [largest] + [least] * (number_of - 1), total - largest - least * (number_of - 1)
    while spare > 0:
        free = [i for i in range(1, number_of) if given[i] < largest] or [i for i in range(1, number_of) if given[i] < bound]
        pool, left = sum([portions[i] for i in free]), spare
        for i in free:
            extra = min(bound - given[i], max(1, left * portions[i] // pool), spare)
            given[i] = given[i] + extra
            spare = spare - extra
    return np.array(given)


def normal_values(rng, shape, deviation, limit, pieces=(), kind=jnp.bfloat16):
    values = deviation * jax.random.normal(rng, shape, jnp.float32)
    if pieces:
        values = values * levels(rng, shape, pieces, -0.22, 0.18)
    return jnp.clip(values, -limit, limit).astype(kind)


def setup_inputs(seed: int = 0, part: int = 0) -> dict:
    key_of = jax.random.split(jax.random.key(seed), 8)
    own_keys = jax.random.split(jax.random.fold_in(key_of[7], part), 8)
    tokens = normal_values(own_keys[0], (TOKENS, D), 1.0, 6.0, ((0, 16),))
    routing_keys = jax.random.split(jax.random.fold_in(own_keys[1], 1), TOKENS // TOK_DEV)
    routing_turns = jax.random.permutation(jax.random.fold_in(own_keys[1], 3), TOKENS // TOK_DEV)
    routing = jax.vmap(lambda own, number: assign_block(jax.random.fold_in(own_keys[1], 2), own, number, TOK_DEV, EXPERTS, TOP, CAP, 2))(routing_keys, routing_turns).reshape((TOKENS, TOP))
    gates = jnp.clip(0.2 + 0.8 * jax.random.uniform(own_keys[2], (TOKENS, TOP), jnp.float32) ** levels(own_keys[2], (TOKENS, TOP), ((0, 16),), -0.2, 0.2), 0.2, 1.0)
    norm_gain = jnp.clip(1.0 + 0.18 * jax.random.normal(key_of[3], (D,), jnp.float32), 0.099609375, 1.8984375).astype(jnp.bfloat16)
    w_gate = normal_values(key_of[4], (N_EP, D, FF // GROUP), D ** -0.5, 0.125, ((0, 16),))
    w_up = normal_values(key_of[5], (N_EP, D, FF // GROUP), D ** -0.5, 0.125, ((0, 16),))
    w_down = normal_values(key_of[6], (N_EP, FF // GROUP, D), FF ** -0.5, 0.09375, ((0, 16),))
    return dict(tokens=tokens, routing=routing, gates=gates, norm_gain=norm_gain, w_gate=w_gate, w_up=w_up, w_down=w_down)


def run_expert(operands):
    expert_rows, gate_piece, up_piece, down_piece = operands
    gate_matrix = jnp.moveaxis(gate_piece, 0, 1).reshape(D, FF)
    up_matrix = jnp.moveaxis(up_piece, 0, 1).reshape(D, FF)
    gate_act = jnp.dot(expert_rows, gate_matrix, preferred_element_type=jnp.float32)
    up_act = jnp.dot(expert_rows, up_matrix, preferred_element_type=jnp.float32)
    hidden = (jax.nn.silu(gate_act) * up_act).astype(jnp.bfloat16)
    return jnp.dot(hidden, down_piece, preferred_element_type=jnp.float32).astype(jnp.bfloat16)

def reference(tokens, routing, gates, norm_gain, w_gate, w_up, w_down):
    values = tokens.astype(jnp.float32)
    scale = lax.rsqrt(lax.optimization_barrier(jnp.mean(values * values, axis=-1, keepdims=True)) + 1e-06)
    normed = (values * scale * norm_gain.astype(jnp.float32)).astype(jnp.bfloat16)
    blocks = routing.reshape(N_EP, TOK_DEV, TOP).astype(jnp.int32)
    one_hot = (blocks[..., None] == jnp.arange(EXPERTS, dtype=jnp.int32)).astype(jnp.int32)
    per_token = lax.optimization_barrier(jnp.sum(one_hot, axis=2)).astype(jnp.int32)
    before = (jnp.cumsum(per_token, axis=1) - per_token).astype(jnp.int32)
    slots = lax.optimization_barrier(jnp.sum(one_hot * before[:, :, None, :], axis=-1)).astype(jnp.int32)
    source = jnp.arange(N_EP, dtype=jnp.int32)[:, None, None]
    target = ((blocks * N_EP + source) * CAP + slots).reshape(-1).astype(jnp.int32)
    filled = jnp.zeros((EXPERTS * N_EP * CAP, D), jnp.bfloat16)
    filled = filled.at[target].set(jnp.repeat(normed, TOP, axis=0))
    expert_rows = filled.reshape(EXPERTS, N_EP * CAP, D)
    gate_pieces = w_gate.reshape(EXPERTS, GROUP, D, FF // GROUP)
    up_pieces = w_up.reshape(EXPERTS, GROUP, D, FF // GROUP)
    down_pieces = w_down.reshape(EXPERTS, FF, D)
    results = lax.map(run_expert, (expert_rows, gate_pieces, up_pieces, down_pieces))
    picked = results.reshape(EXPERTS * N_EP * CAP, D)[target].reshape(N_EP * TOK_DEV, TOP, D)
    mixed = lax.optimization_barrier(jnp.sum(gates[..., None] * picked.astype(jnp.float32), axis=1))
    return mixed.astype(jnp.bfloat16)
```

```python
import functools

import jax
import jax.numpy as jnp
from jax import lax
from jax.experimental import pallas as pl
from jax.experimental.pallas import tpu as pltpu
from jax.sharding import PartitionSpec as P

GROUP = 4
LANE = 128


def kernel(n, cap, tok, rt, gt, gain, wg, wu, wd, out,
           normed, outgoing, xbuf, wgu, wdn, hidden, part, give, take, cross, crossed,
           finished, ret, total, w_sem, zs, zr, ys, yr, cs, cr, fs, fr, gs, gr, bs, br, es, er):
    toks, width = tok.shape
    ff = wg.shape[1]
    me = lax.axis_index("ep")
    g, j = me // GROUP, me % GROUP
    partner = g * GROUP + (j + 1 - 2 * (j % 2))
    across = g * GROUP + (j + 2) % GROUP
    sign = jnp.where(g < n // 2, 1, -1)
    offsets = list(range(n // 2, n)) + list(range(n // 2 - 1, 0, -1))

    def peer(offset):
        return (g + sign * offset + n) % n

    sources = [g] + [peer(o) for o in offsets]

    def remote(src, dst, send, recv, device):
        return pltpu.make_async_remote_copy(
            src_ref=src, dst_ref=dst, send_sem=send, recv_sem=recv,
            device_id={"ep": device}, device_id_type=pl.DeviceIdType.MESH)

    barrier = pltpu.get_barrier_semaphore()
    others = [partner, across] + [s * GROUP + j for s in sources[1:]]
    for other in others:
        pl.semaphore_signal(barrier, inc=1, device_id={"ep": other},
                            device_id_type=pl.DeviceIdType.MESH)

    tiles = ff // LANE
    loads = []
    for t in range(tiles):
        loads.append(pltpu.make_async_copy(wg.at[:, pl.ds(t * LANE, LANE)], wgu.at[t, :, pl.ds(0, LANE)], w_sem.at[2 * t]))
        loads.append(pltpu.make_async_copy(wu.at[:, pl.ds(t * LANE, LANE)], wgu.at[t, :, pl.ds(LANE, LANE)], w_sem.at[2 * t + 1]))
    loads.append(pltpu.make_async_copy(wd, wdn, w_sem.at[2 * tiles]))
    for load in loads:
        load.start()

    values = tok[...].astype(jnp.float32)
    scale = lax.rsqrt(jnp.mean(values * values, axis=-1, keepdims=True) + 1e-06)
    normed[...] = (values * scale * gain[...].astype(jnp.float32)).astype(jnp.bfloat16)

    first, second = rt[:, 0:1], rt[:, 1:2]
    experts_at = lax.broadcasted_iota(jnp.int32, (toks, LANE), 1)
    named = ((experts_at == first) | (experts_at == second)).astype(jnp.float32)
    lower = (lax.broadcasted_iota(jnp.int32, (toks, toks), 1)
             < lax.broadcasted_iota(jnp.int32, (toks, toks), 0)).astype(jnp.bfloat16)
    before = jnp.dot(lower, named.astype(jnp.bfloat16), preferred_element_type=jnp.float32)
    code = jnp.where(named > 0.5, before, -1.0)
    code_t = code.T

    def pack(e, dst):
        row = jnp.sum(jnp.where(lax.broadcasted_iota(jnp.int32, (LANE, toks), 0) == e, code_t, 0.0), axis=0, keepdims=True)
        slot = lax.broadcasted_iota(jnp.int32, (cap, toks), 0).astype(jnp.float32)
        pick = (slot == row).astype(jnp.bfloat16)

        def body(t, _):
            cols = pl.ds(pl.multiple_of(t * 512, 512), 512)
            dst[:, cols] = jnp.dot(pick, normed[:, cols], preferred_element_type=jnp.float32).astype(jnp.bfloat16)
            return _

        lax.fori_loop(0, width // 512, body, 0)

    def lane_rows(lane):
        return pl.ds(lane * cap, cap)

    waits = []

    def share_copies(i):
        s = sources[i]
        return [remote(xbuf.at[s, lane_rows(0)], xbuf.at[s, lane_rows(2)], ys.at[i], yr.at[i], across),
                remote(xbuf.at[s, lane_rows(0)], xbuf.at[s, lane_rows(1)], cs.at[i], cr.at[i], partner)]

    def forward_copy(i):
        s = sources[i]
        return remote(xbuf.at[s, lane_rows(2)], xbuf.at[s, lane_rows(3)], fs.at[i], fr.at[i], partner)

    def give_copy(i):
        return remote(give.at[i], take.at[i], gs.at[i], gr.at[i], partner)

    def cross_copy(i):
        return remote(cross.at[i], crossed.at[i], bs.at[i], br.at[i], across)

    def arrive(i):
        if i:
            s = sources[i]
            remote(outgoing.at[0], xbuf.at[s, lane_rows(0)], zs.at[0], zr.at[s], partner).wait_recv()
        for copy in share_copies(i):
            copy.start()
            waits.append(copy)

    def forward(i):
        share_copies(i)[0].wait_recv()
        copy = forward_copy(i)
        copy.start()
        waits.append(copy)

    def compute(i):
        s, slot = sources[i], i % 2
        share_copies(i)[1].wait_recv()
        forward_copy(i).wait_recv()

        def up(t, _):
            both = jnp.dot(xbuf[s], wgu[t], preferred_element_type=jnp.float32)
            gate_act, up_act = both[:, :LANE], both[:, LANE:]
            act = gate_act / (1.0 + jnp.exp(-gate_act)) * up_act
            hidden[:, pl.ds(pl.multiple_of(t * LANE, LANE), LANE)] = act.astype(jnp.bfloat16)
            return _

        lax.fori_loop(0, tiles, up, 0)

        def down(t, _):
            cols = pl.ds(pl.multiple_of(t * 256, 256), 256)
            piece = jnp.dot(hidden[...], wdn[:, cols], preferred_element_type=jnp.float32)
            part[slot, 0, :, cols] = piece[0:cap]
            give[i, 0, :, cols] = piece[cap:2 * cap].astype(jnp.bfloat16)
            part[slot, 1, :, cols] = piece[2 * cap:3 * cap]
            give[i, 1, :, cols] = piece[3 * cap:4 * cap].astype(jnp.bfloat16)
            return _

        lax.fori_loop(0, width // 256, down, 0)
        copy = give_copy(i)
        copy.start()
        waits.append(copy)

    def reduce_pair(i):
        give_copy(i).wait_recv()
        cross[i] = (part[i % 2, 1] + take[i, 1].astype(jnp.float32)).astype(jnp.bfloat16)
        copy = cross_copy(i)
        copy.start()
        waits.append(copy)

    def finish(i):
        cross_copy(i).wait_recv()
        done = (part[i % 2, 0] + take[i, 0].astype(jnp.float32) + crossed[i].astype(jnp.float32)).astype(jnp.bfloat16)
        if i == 0:
            ret[g] = done
        else:
            finished[i] = done
            copy = remote(finished.at[i], ret.at[g], es.at[i], er.at[g], sources[i] * GROUP + j)
            copy.start()
            waits.append(copy)

    def mix(i):
        e = sources[i]
        if i:
            remote(finished.at[i], ret.at[e], es.at[i], er.at[e], partner).wait_recv()
        column = jnp.sum(jnp.where(experts_at == e, code, 0.0), axis=1, keepdims=True)
        slot = lax.broadcasted_iota(jnp.int32, (toks, cap), 1).astype(jnp.float32)
        pick = (slot == column).astype(jnp.bfloat16)
        gate = jnp.where(first == e, gt[:, 0:1], 0.0) + jnp.where(second == e, gt[:, 1:2], 0.0)

        def body(t, _):
            cols = pl.ds(pl.multiple_of(t * 512, 512), 512)
            term = gate * jnp.dot(pick, ret[e, :, cols], preferred_element_type=jnp.float32)
            if i:
                term = total[:, cols] + term
            if i == n - 1:
                out[:, cols] = term.astype(jnp.bfloat16)
            else:
                total[:, cols] = term
            return _

        lax.fori_loop(0, width // 512, body, 0)

    pack(g, xbuf.at[g, lane_rows(0)])
    pack(sources[1], outgoing.at[1])
    pl.semaphore_wait(barrier, len(others))
    arrive(0)
    for i in range(1, n):
        if i > 1:
            pack(sources[i], outgoing.at[i])
        copy = remote(outgoing.at[i], xbuf.at[g, lane_rows(0)], zs.at[i], zr.at[g], sources[i] * GROUP + j)
        copy.start()
        waits.append(copy)
    forward(0)
    arrive(1)
    for load in loads:
        load.wait()
    for i in range(n):
        compute(i)
        if i:
            finish(i - 1)
        reduce_pair(i)
        if i + 1 < n:
            forward(i + 1)
        if i + 2 < n:
            arrive(i + 2)
    mix(0)
    if n > 2:
        mix(1)
    finish(n - 1)
    for i in range(2 if n > 2 else 1, n):
        mix(i)
    for copy in waits:
        copy.wait_send()


def per_device(tokens, routing, gates, norm_gain, w_gate, w_up, w_down):
    toks, width = tokens.shape
    top = routing.shape[1]
    devices = lax.axis_size("ep")
    n = devices // GROUP
    cap = GROUP * (5 * toks * top // (4 * devices))
    cap = -(-cap // 16) * 16
    ff = w_gate.shape[2]
    bf, f32 = jnp.bfloat16, jnp.float32
    dma = pltpu.SemaphoreType.DMA((n,))
    vmem = pl.BlockSpec(memory_space=pltpu.VMEM)
    hbm = pl.BlockSpec(memory_space=pl.ANY)
    return pl.pallas_call(
        functools.partial(kernel, n, cap),
        out_shape=jax.ShapeDtypeStruct((toks, width), bf),
        in_specs=[vmem] * 4 + [hbm] * 3,
        out_specs=vmem,
        scratch_shapes=[
            pltpu.VMEM((toks, width), bf),
            pltpu.VMEM((n, cap, width), bf),
            pltpu.VMEM((n, GROUP * cap, width), bf),
            pltpu.VMEM((ff // LANE, width, 2 * LANE), bf),
            pltpu.VMEM((ff, width), bf),
            pltpu.VMEM((GROUP * cap, ff), bf),
            pltpu.VMEM((2, 2, cap, width), f32),
            pltpu.VMEM((n, 2, cap, width), bf),
            pltpu.VMEM((n, 2, cap, width), bf),
            pltpu.VMEM((n, cap, width), bf),
            pltpu.VMEM((n, cap, width), bf),
            pltpu.VMEM((n, cap, width), bf),
            pltpu.VMEM((n, cap, width), bf),
            pltpu.VMEM((toks, width), f32),
            pltpu.SemaphoreType.DMA((2 * (ff // LANE) + 1,)),
        ] + [dma] * 14,
        compiler_params=pltpu.CompilerParams(
            collective_id=0, has_side_effects=True, vmem_limit_bytes=62 * 1024 * 1024),
    )(tokens, routing, gates, norm_gain.reshape(1, width), w_gate.reshape(w_gate.shape[1:]),
      w_up.reshape(w_up.shape[1:]), w_down.reshape(w_down.shape[1:]))


def solution(mesh):
    placed = (
        P(("grp", "ep"), None),
        P(("grp", "ep"), None),
        P(("grp", "ep"), None),
        P(),
        P("ep", None, None),
        P("ep", None, None),
        P("ep", None, None),
    )
    return jax.shard_map(
        per_device, mesh=mesh, in_specs=placed, out_specs=P(("grp", "ep"), None), check_vma=False
    )
```

```python
import functools

import jax
import jax.numpy as jnp
from jax import lax
from jax.experimental import pallas as pl
from jax.experimental.pallas import tpu as pltpu
from jax.sharding import PartitionSpec as P

GROUP = 4
LANE = 128
PIECES = 4


def kernel(n, cap, tok, rt, gt, gain, wg, wu, wd, out,
           normed, outgoing, xbuf, wgu, wdn, hidden, part, give, take, cross, crossed,
           finished, ret, total, table, w_sem, zs, zr, ys, yr, cs, cr, fs, fr, gs, gr, bs, br, es, er):
    toks, width = tok.shape
    ff = wg.shape[1]
    me = lax.axis_index("ep")
    g, j = me // GROUP, me % GROUP
    partner = g * GROUP + (j + 1 - 2 * (j % 2))
    across = g * GROUP + (j + 2) % GROUP
    sources = [(g + o) % n for o in range(n)]
    send_order = sorted(range(1, n), key=lambda o: min(o, n - o))
    span = width // PIECES

    def remote(src, dst, send, recv, device):
        return pltpu.make_async_remote_copy(
            src_ref=src, dst_ref=dst, send_sem=send, recv_sem=recv,
            device_id={"ep": device}, device_id_type=pl.DeviceIdType.MESH)

    barrier = pltpu.get_barrier_semaphore()
    others = [partner, across] + [s * GROUP + j for s in sources[1:]]
    for other in others:
        pl.semaphore_signal(barrier, inc=1, device_id={"ep": other},
                            device_id_type=pl.DeviceIdType.MESH)

    tiles = ff // LANE
    loads = []
    for t in range(tiles):
        loads.append(pltpu.make_async_copy(wg.at[:, pl.ds(t * LANE, LANE)], wgu.at[t, :, pl.ds(0, LANE)], w_sem.at[2 * t]))
        loads.append(pltpu.make_async_copy(wu.at[:, pl.ds(t * LANE, LANE)], wgu.at[t, :, pl.ds(LANE, LANE)], w_sem.at[2 * t + 1]))
    loads.append(pltpu.make_async_copy(wd, wdn, w_sem.at[2 * tiles]))
    for load in loads:
        load.start()

    values = tok[...].astype(jnp.float32)
    scale = lax.rsqrt(jnp.mean(values * values, axis=-1, keepdims=True) + 1e-06)
    normed[...] = (values * scale * gain[...].reshape(1, width).astype(jnp.float32)).astype(jnp.bfloat16)

    table[...] = jnp.zeros_like(table)
    table[0:2] = rt[...].astype(jnp.float32)
    table[2:4] = gt[...]
    turned = table[...].T
    first, second = turned[:, 0:1], turned[:, 1:2]
    experts_at = lax.broadcasted_iota(jnp.int32, (toks, LANE), 1).astype(jnp.float32)
    named = ((experts_at == first) | (experts_at == second)).astype(jnp.float32)
    lower = (lax.broadcasted_iota(jnp.int32, (toks, toks), 1)
             < lax.broadcasted_iota(jnp.int32, (toks, toks), 0)).astype(jnp.bfloat16)
    before = jnp.dot(lower, named.astype(jnp.bfloat16), preferred_element_type=jnp.float32)
    code = jnp.where(named > 0.5, before, -1.0)
    code_t = code.T

    def pack(e, dst):
        row = jnp.sum(jnp.where(lax.broadcasted_iota(jnp.int32, (LANE, toks), 0) == e, code_t, 0.0), axis=0, keepdims=True)
        slot = lax.broadcasted_iota(jnp.int32, (cap, toks), 0).astype(jnp.float32)
        pick = (slot == row).astype(jnp.bfloat16)

        def body(t, _):
            cols = pl.ds(pl.multiple_of(t * 512, 512), 512)
            dst[:, cols] = jnp.dot(pick, normed[:, cols], preferred_element_type=jnp.float32).astype(jnp.bfloat16)
            return _

        lax.fori_loop(0, width // 512, body, 0)

    def lane_rows(lane):
        return pl.ds(lane * cap, cap)

    waits = []

    def start(copy):
        copy.start()
        waits.append(copy)

    def across_copy(i):
        s = sources[i]
        return remote(xbuf.at[s, lane_rows(0)], xbuf.at[s, lane_rows(2)], ys.at[i], yr.at[i], across)

    def beside_copy(i):
        s = sources[i]
        return remote(xbuf.at[s, lane_rows(0)], xbuf.at[s, lane_rows(1)], cs.at[i], cr.at[i], partner)

    def forward_copy(i):
        s = sources[i]
        return remote(xbuf.at[s, lane_rows(2)], xbuf.at[s, lane_rows(3)], fs.at[i], fr.at[i], partner)

    def piece_of(h):
        return pl.ds(h * span, span)

    def give_copy(i, h):
        return remote(give.at[i, :, :, piece_of(h)], take.at[i, :, :, piece_of(h)],
                      gs.at[i, h], gr.at[i, h], partner)

    def cross_copy(i, h):
        return remote(cross.at[i, :, piece_of(h)], crossed.at[i, :, piece_of(h)],
                      bs.at[i, h], br.at[i, h], across)

    def arrive(i):
        if i:
            s = sources[i]
            remote(outgoing.at[0], xbuf.at[s, lane_rows(0)], zs.at[0], zr.at[s], partner).wait_recv()
        start(across_copy(i))
        start(beside_copy(i))

    def forward(i):
        across_copy(i).wait_recv()
        start(forward_copy(i))

    def rise(i):
        s = sources[i]
        beside_copy(i).wait_recv()
        forward_copy(i).wait_recv()

        def up(t, _):
            both = jnp.dot(xbuf[s], wgu[t], preferred_element_type=jnp.float32)
            gate_act, up_act = both[:, :LANE], both[:, LANE:]
            act = gate_act / (1.0 + jnp.exp(-gate_act)) * up_act
            hidden[:, pl.ds(pl.multiple_of(t * LANE, LANE), LANE)] = act.astype(jnp.bfloat16)
            return _

        lax.fori_loop(0, tiles, up, 0)

    def fall(i, h):
        slot = i % 2

        def down(t, _):
            cols = pl.ds(pl.multiple_of(h * span + t * 256, 256), 256)
            piece = jnp.dot(hidden[...], wdn[:, cols], preferred_element_type=jnp.float32)
            part[slot, 0, :, cols] = piece[0:cap]
            give[i, 0, :, cols] = piece[cap:2 * cap].astype(jnp.bfloat16)
            part[slot, 1, :, cols] = piece[2 * cap:3 * cap]
            give[i, 1, :, cols] = piece[3 * cap:4 * cap].astype(jnp.bfloat16)
            return _

        lax.fori_loop(0, span // 256, down, 0)
        start(give_copy(i, h))

    def reduce_pair(i, h):
        give_copy(i, h).wait_recv()
        cols = piece_of(h)
        cross[i, :, cols] = (part[i % 2, 1, :, cols] + take[i, 1, :, cols].astype(jnp.float32)).astype(jnp.bfloat16)
        start(cross_copy(i, h))

    def finish(i, h):
        cross_copy(i, h).wait_recv()
        cols = piece_of(h)
        done = (part[i % 2, 0, :, cols] + take[i, 0, :, cols].astype(jnp.float32)
                + crossed[i, :, cols].astype(jnp.float32)).astype(jnp.bfloat16)
        if i == 0:
            ret[g, :, cols] = done
        else:
            finished[i, :, cols] = done
            start(remote(finished.at[i, :, cols], ret.at[g, :, cols], es.at[i, h], er.at[g, h],
                         sources[i] * GROUP + j))

    def mix(i, h, last):
        e = sources[i]
        cols = piece_of(h)
        if i:
            remote(finished.at[i, :, cols], ret.at[e, :, cols], es.at[i, h], er.at[e, h], partner).wait_recv()
        column = jnp.sum(jnp.where(experts_at == e.astype(jnp.float32), code, 0.0), axis=1, keepdims=True)
        slot = lax.broadcasted_iota(jnp.int32, (toks, cap), 1).astype(jnp.float32)
        pick = (slot == column).astype(jnp.bfloat16)
        name = e.astype(jnp.float32)
        gate = jnp.where(first == name, turned[:, 2:3], 0.0) + jnp.where(second == name, turned[:, 3:4], 0.0)
        term = gate * jnp.dot(pick, ret[e, :, cols], preferred_element_type=jnp.float32)
        if i:
            term = total[:, cols] + term
        if last:
            out[:, cols] = term.astype(jnp.bfloat16)
        else:
            total[:, cols] = term

    pieces = range(PIECES)
    pack(g, xbuf.at[g, lane_rows(0)])
    pack(sources[send_order[0]], outgoing.at[send_order[0]])
    pl.semaphore_wait(barrier, len(others))
    arrive(0)
    for o in send_order:
        if o != send_order[0]:
            pack(sources[o], outgoing.at[o])
        start(remote(outgoing.at[o], xbuf.at[g, lane_rows(0)], zs.at[o], zr.at[g], sources[o] * GROUP + j))
    forward(0)
    arrive(1)
    for load in loads:
        load.wait()
    for i in range(n):
        rise(i)
        if i and i + 1 < n:
            arrive(i + 1)
        for h in pieces:
            fall(i, h)
            if h:
                reduce_pair(i, h - 1)
        reduce_pair(i, PIECES - 1)
        if i:
            for h in pieces:
                finish(i - 1, h)
        if i + 1 < n:
            forward(i + 1)
    order = [0] + [n - o for o in range(1, n)]
    for i in order[:-1]:
        if i == order[-2]:
            for h in pieces:
                finish(n - 1, h)
        for h in pieces:
            mix(i, h, False)
    for h in pieces:
        mix(order[-1], h, True)
    for copy in waits:
        copy.wait_send()


def per_device(tokens, routing, gates, norm_gain, w_gate, w_up, w_down):
    toks, width = tokens.shape
    top = routing.shape[1]
    devices = lax.axis_size("ep")
    n = devices // GROUP
    cap = GROUP * (5 * toks * top // (4 * devices))
    cap = -(-cap // 16) * 16
    ff = w_gate.shape[2]
    bf, f32 = jnp.bfloat16, jnp.float32
    dma = pltpu.SemaphoreType.DMA((n,))
    dmas = pltpu.SemaphoreType.DMA((n, PIECES))
    vmem = pl.BlockSpec(memory_space=pltpu.VMEM)
    hbm = pl.BlockSpec(memory_space=pl.ANY)
    return pl.pallas_call(
        functools.partial(kernel, n, cap),
        out_shape=jax.ShapeDtypeStruct((toks, width), bf),
        in_specs=[vmem] * 4 + [hbm] * 3,
        out_specs=vmem,
        scratch_shapes=[
            pltpu.VMEM((toks, width), bf),
            pltpu.VMEM((n, cap, width), bf),
            pltpu.VMEM((n, GROUP * cap, width), bf),
            pltpu.VMEM((ff // LANE, width, 2 * LANE), bf),
            pltpu.VMEM((ff, width), bf),
            pltpu.VMEM((GROUP * cap, ff), bf),
            pltpu.VMEM((2, 2, cap, width), f32),
            pltpu.VMEM((n, 2, cap, width), bf),
            pltpu.VMEM((n, 2, cap, width), bf),
            pltpu.VMEM((n, cap, width), bf),
            pltpu.VMEM((n, cap, width), bf),
            pltpu.VMEM((n, cap, width), bf),
            pltpu.VMEM((n, cap, width), bf),
            pltpu.VMEM((toks, width), f32),
            pltpu.VMEM((LANE, toks), f32),
            pltpu.SemaphoreType.DMA((2 * (ff // LANE) + 1,)),
        ] + [dma] * 8 + [dmas] * 6,
        compiler_params=pltpu.CompilerParams(
            collective_id=0, has_side_effects=True, vmem_limit_bytes=62 * 1024 * 1024),
    )(tokens, routing.T, gates.T, norm_gain, w_gate.reshape(w_gate.shape[1:]),
      w_up.reshape(w_up.shape[1:]), w_down.reshape(w_down.shape[1:]))


def solution(mesh):
    placed = (
        P(("grp", "ep"), None),
        P(("grp", "ep"), None),
        P(("grp", "ep"), None),
        P(),
        P("ep", None, None),
        P("ep", None, None),
        P("ep", None, None),
    )
    return jax.shard_map(
        per_device, mesh=mesh, in_specs=placed, out_specs=P(("grp", "ep"), None), check_vma=False
    )
```
